256 devices in a mesh: sp: 32 (over z, y), dp: 8 (over x, core).
Axes of the slice: x: 4, y: 4, z: 8, core: 2. Of those that a mesh axis runs over, the one named last changes fastest.
Arguments:
- queries: bfloat16 [32768, 6144], P(('dp', 'sp')), may hold values from -360 to 360
- latent: bfloat16 [32768, 1024], P(('dp', 'sp')), may hold values from -6 to 6
- rope_key: bfloat16 [32768, 64], P(('dp', 'sp')), may hold values from -6 to 6
- latent_gain: float32 [1024], replicated, may hold values from 0.1 to 1.9
- kv_weight: bfloat16 [1024, 8192], P(None, 'dp'), may hold values from -0.1875 to 0.1875
- gate: bfloat16 [32768, 4096], P(('dp', 'sp')), may hold values from -6 to 6
- out_gain: float32 [4096], replicated, may hold values from 0.1 to 1.9
Outputs:
- attended: bfloat16 [32768, 4096], P(('dp', 'sp'))
The draws below stay inside these ranges and needn't reach their ends.
All inputs are finite; a program needn't handle non-finite values.
Results may differ from the reference program's by a relative error of at most 0.007.
Values may be sent and summed in bfloat16 or wider, within the bound.
No kernel may reach another device: no remote copies, remote signals or barrier semaphores. Data moves between devices by JAX's collectives and lax.ppermute only.
A program may use at most 128 MiB of HBM per device.

```python
import jax
import jax.numpy as jnp
from jax import lax

HEADS = 32
NOPE = 128
ROPE = 64
VDIM = 128
KV_RANK = 1024
SEQ_LEN = 4096
TOKENS = 32768


def draw_queries(key, part):
    values = jax.random.normal(key, (TOKENS, HEADS * (NOPE + ROPE)), jnp.float32)
    values = jnp.clip(values, -6.0, 6.0)
    return values.astype(jnp.bfloat16)


def steps_of(stream_key, extent, shards, low, largest):
    loudness = 1.0
    for dim, blocks in shards:
        steps = jax.random.uniform(jax.random.fold_in(jax.random.fold_in(stream_key, 6), dim), (blocks,), jnp.float32, low / len(shards), largest / len(shards))
        loudness = loudness * jnp.repeat(jnp.exp(steps), extent[dim] // blocks).reshape((-1,) + (1,) * (len(extent) - 1 - dim))
    return loudness


def bell_draw(own_key, shape, spread, limit, pieces=(), held_as=jnp.bfloat16):
    loudness = steps_of(own_key, shape, pieces, -0.22, 0.18) if pieces else 1.0
    values = jax.random.normal(own_key, shape, jnp.float32) * spread * loudness
    return jnp.minimum(jnp.maximum(values, -limit), limit).astype(held_as)


def setup_inputs(seed: int = 0) -> dict:
    streams_of = jax.random.split(jax.random.key(seed), 8)
    return {
        "queries": draw_queries(jax.random.fold_in(streams_of[7], 71), 0),
        "latent": bell_draw(streams_of[1], (TOKENS, KV_RANK), 1.0, 6.0, ((0, 256),)),
        "rope_key": bell_draw(streams_of[2], (TOKENS, ROPE), 1.0, 6.0, ((0, 256),)),
        "latent_gain": jnp.clip(1.0 + 0.18 * jax.random.normal(streams_of[3], (KV_RANK,), jnp.float32), 0.1, 1.9),
        "kv_weight": bell_draw(streams_of[4], (KV_RANK, HEADS * (NOPE + VDIM)), KV_RANK ** -0.5, 0.1875, ((1, 8),)),
        "gate": bell_draw(streams_of[5], (TOKENS, HEADS * VDIM), 1.0, 6.0, ((0, 256),)),
        "out_gain": jnp.clip(1.0 + 0.18 * jax.random.normal(streams_of[6], (HEADS * VDIM,), jnp.float32), 0.1, 1.9),
    }


EPS = 1e-06
THETA = 10000.0

def rotary(values, position):
    half_width = values.shape[-1] // 2
    inverse = THETA ** (-jnp.arange(half_width, dtype=jnp.float32) / half_width)
    angles = position.astype(jnp.float32)[:, None] * inverse[None, :]
    if values.ndim == 3:
        angles = angles[:, None, :]
    cosine = jnp.cos(angles)
    sine_part = jnp.sin(angles)
    front_half = values[..., :half_width].astype(jnp.float32)
    back_half = values[..., half_width:].astype(jnp.float32)
    turned = jnp.concatenate([front_half * cosine - back_half * sine_part, back_half * cosine + front_half * sine_part], axis=-1)
    return turned.astype(jnp.bfloat16)

def attend(query_block, keys_plain, keys_rotated, values):
    scores = jnp.einsum('qhd,khd->hqk', query_block[..., :NOPE].astype(jnp.float32), keys_plain.astype(jnp.float32))
    scores = scores + jnp.einsum('qhr,kr->hqk', query_block[..., NOPE:].astype(jnp.float32), keys_rotated.astype(jnp.float32))
    scores = scores * (NOPE + ROPE) ** (-0.5)
    row_max = lax.optimization_barrier(jnp.max(scores, axis=-1, keepdims=True))
    raised = jnp.exp(scores - row_max)
    weights = (raised / lax.optimization_barrier(jnp.sum(raised, axis=-1, keepdims=True))).astype(jnp.bfloat16)
    result = jnp.einsum('hqk,khd->qhd', weights.astype(jnp.float32), values.astype(jnp.float32))
    return result.astype(jnp.bfloat16)

def reference(queries, latent, rope_key, latent_gain, kv_weight, gate, out_gain):
    rows_all = queries.shape[0]
    position = jnp.arange(rows_all, dtype=jnp.int32) % SEQ_LEN
    widened = latent.astype(jnp.float32)
    normed = (widened * lax.rsqrt(lax.optimization_barrier(jnp.mean(widened * widened, axis=-1, keepdims=True)) + EPS) * latent_gain.astype(jnp.float32)).astype(jnp.bfloat16)
    keyval = jnp.dot(normed, kv_weight, preferred_element_type=jnp.float32).astype(jnp.bfloat16)
    head_queries = queries.reshape(rows_all, HEADS, NOPE + ROPE)
    head_queries = jnp.concatenate([head_queries[..., :NOPE], rotary(head_queries[..., NOPE:], position)], axis=-1)
    keys_rotated = rotary(rope_key, position)
    seq_count = rows_all // SEQ_LEN
    block_rows = min(512, SEQ_LEN)
    block_count = SEQ_LEN // block_rows

    def one_sequence(operands):
        query_seq, kv_seq, rope_seq = operands
        keys_plain = kv_seq[..., :NOPE]
        values = kv_seq[..., NOPE:]
        blocks = query_seq.reshape(block_count, block_rows, HEADS, NOPE + ROPE)
        result = lax.map(lambda piece_rows: attend(piece_rows, keys_plain, rope_seq, values), blocks)
        return result.reshape(SEQ_LEN, HEADS * VDIM)
    heads_out = lax.map(one_sequence, (head_queries.reshape(seq_count, SEQ_LEN, HEADS, NOPE + ROPE), keyval.reshape(seq_count, SEQ_LEN, HEADS, NOPE + VDIM), keys_rotated.reshape(seq_count, SEQ_LEN, ROPE)))
    heads_out = heads_out.reshape(rows_all, HEADS * VDIM)
    gated_rows = heads_out.astype(jnp.float32) * jax.nn.silu(gate.astype(jnp.float32))
    scale_rows = lax.rsqrt(lax.optimization_barrier(jnp.mean(gated_rows * gated_rows, axis=-1, keepdims=True)) + EPS)
    return (gated_rows * scale_rows * out_gain.astype(jnp.float32)).astype(jnp.bfloat16)
```

```python
import functools
import math

import jax
import jax.numpy as jnp
from jax import lax
from jax.experimental import pallas as pl
from jax.experimental.pallas import tpu as pltpu
from jax.sharding import Mesh
from jax.sharding import PartitionSpec as P

HEADS = 32
NOPE = 128
ROPE = 64
VDIM = 128
RANK = 1024
GROUPS = 8
PER = HEADS // GROUPS
OWN = 128
QCOLS = PER * (NOPE + ROPE)
WIDE = RANK + 2 * ROPE

EPS = 1e-06
THETA = 10000.0
SCALE2 = math.log2(math.e) / math.sqrt(NOPE + ROPE)
F32 = jnp.float32
BF16 = jnp.bfloat16

Z = ("zh", "zl")
DP = ("x", "core")
EVERY = ("zh", "zl", "y", "x", "core")


def turned(pair, cosine, signed_sine):
    u = pair.astype(F32)
    first = lax.broadcasted_iota(jnp.int32, u.shape, 1) % ROPE < ROPE // 2
    partner = jnp.where(first, pltpu.roll(u, 128 - ROPE // 2, 1), pltpu.roll(u, ROPE // 2, 1))
    return (u * cosine + partner * signed_sine).astype(BF16)


def latent_kernel(latent_ref, key_ref, gain_ref, cos_ref, sin_ref, sent_ref):
    wide = latent_ref[...].astype(F32)
    mean = jnp.mean(wide * wide, axis=-1, keepdims=True)
    sent_ref[:, :RANK] = (wide * lax.rsqrt(mean + EPS) * gain_ref[...]).astype(BF16)
    key = key_ref[...]
    sent_ref[:, RANK:] = turned(jnp.concatenate([key, key], axis=1), cos_ref[...], sin_ref[...])


def query_kernel(q_ref, cos_ref, sin_ref, sent_ref):
    cosine, signed_sine = cos_ref[...], sin_ref[...]
    for pair in range(HEADS // 2):
        group, local = pair // (PER // 2), pair % (PER // 2)
        a, b, c = (q_ref[:, 384 * pair + 128 * i : 384 * pair + 128 * (i + 1)] for i in range(3))
        sent_ref[group, :, 256 * local : 256 * local + 128] = a
        sent_ref[group, :, 256 * local + 128 : 256 * local + 256] = jnp.concatenate(
            [b[:, 64:], c[:, :64]], axis=1
        )
        rope = jnp.concatenate([b[:, :64], c[:, 64:]], axis=1)
        base = PER * NOPE + 128 * local
        sent_ref[group, :, base : base + 128] = turned(rope, cosine, signed_sine)


def small_call(kernel, shape, flops, moved):
    return pl.pallas_call(
        kernel,
        out_shape=jax.ShapeDtypeStruct(shape, BF16),
        cost_estimate=pl.CostEstimate(flops=flops, bytes_accessed=moved, transcendentals=0),
    )


def attention_kernel(sizes, bq, bk, q_ref, *refs):
    pieces, (w_ref, o_ref, kext, vt, acc, m_ref, s_ref) = refs[: len(sizes)], refs[len(sizes) :]
    seq = kext.shape[0]
    h = pl.program_id(0)
    lane = lax.broadcasted_iota(jnp.int32, (1, 128), 1)
    keep = (lane >= ROPE) == (h % 2 == 1)

    @pl.when(h == 0)
    def _():
        row = lax.broadcasted_iota(jnp.int32, (16, seq), 0)
        vt[VDIM:, :] = jnp.where(row == 0, 1.0, 0.0).astype(BF16)

    start = 0
    for size, piece in zip(sizes, pieces):
        rows = pl.ds(start, size)
        kv = jnp.dot(piece[:, :RANK], w_ref[...], preferred_element_type=F32)
        kext[rows, :NOPE] = kv[:, :NOPE].astype(BF16)
        rotated = piece[:, RANK:]
        kext[rows, NOPE:] = jnp.where(keep, rotated, jnp.zeros_like(rotated))
        vt[:VDIM, rows] = kv[:, NOPE:].T.astype(BF16)
        start += size

    blocks = seq // bk
    plain = pl.ds(pl.multiple_of(h * NOPE, 128), 128)
    rope = pl.ds(pl.multiple_of(PER * NOPE + (h // 2) * 128, 128), 128)

    def query_block(qb, carry):
        sources = pl.ds(qb * (bq // OWN), bq // OWN)
        q = jnp.concatenate(
            [q_ref[sources, :, plain].reshape(bq, 128), q_ref[sources, :, rope].reshape(bq, 128)],
            axis=1,
        )

        def score(kb):
            rows = pl.ds(pl.multiple_of(kb * bk, bk), bk)
            return lax.dot_general(
                kext[rows, :], q, (((1,), (1,)), ((), ())), preferred_element_type=F32
            )

        m_ref[...] = jnp.full_like(m_ref, -jnp.inf)
        acc[...] = jnp.zeros_like(acc)
        s_ref[0] = score(0)

        def step(kb, slot):
            s_ref[1 - slot] = score(jnp.minimum(kb + 1, blocks - 1))
            s = s_ref[slot]
            m_old = m_ref[0:1, :]
            m_new = jnp.maximum(m_old, jnp.max(s, axis=0, keepdims=True))
            p = jnp.exp2((s - m_new) * SCALE2).astype(BF16)
            shrink = jnp.exp2((m_old - m_new) * SCALE2)
            rows = pl.ds(pl.multiple_of(kb * bk, bk), bk)
            acc[...] = acc[...] * shrink + jnp.dot(vt[:, rows], p, preferred_element_type=F32)
            m_ref[0:1, :] = m_new

        def two(i, inner):
            step(2 * i, 0)
            step(2 * i + 1, 1)
            return inner

        lax.fori_loop(0, blocks // 2, two, 0)
        out = (acc[:VDIM, :] / acc[VDIM : VDIM + 1, :]).T.astype(BF16)
        o_ref[sources, :, :] = out.reshape(bq // OWN, OWN, VDIM)
        return carry

    lax.fori_loop(0, GROUPS * OWN // bq, query_block, 0)


def attention(queries, pieces, weight, bq=512, bk=1024):
    sizes = tuple(p.shape[0] for p in pieces)
    seq = sum(sizes)
    rows = GROUPS * OWN
    flops = 2 * PER * (seq * RANK * 256 + rows * seq * 400)
    return pl.pallas_call(
        functools.partial(attention_kernel, sizes, bq, bk),
        grid=(PER,),
        in_specs=[pl.BlockSpec((GROUPS, OWN, QCOLS), lambda h: (0, 0, 0))]
        + [pl.BlockSpec((s, WIDE), lambda h: (0, 0)) for s in sizes]
        + [pl.BlockSpec((RANK, NOPE + VDIM), lambda h: (0, h))],
        out_specs=pl.BlockSpec((GROUPS, OWN, VDIM), lambda h: (0, 0, h)),
        out_shape=jax.ShapeDtypeStruct((GROUPS, OWN, PER * VDIM), BF16),
        scratch_shapes=[
            pltpu.VMEM((seq, 256), BF16),
            pltpu.VMEM((VDIM + 16, seq), BF16),
            pltpu.VMEM((VDIM + 16, bq), F32),
            pltpu.VMEM((8, bq), F32),
            pltpu.VMEM((2, bk, bq), F32),
        ],
        cost_estimate=pl.CostEstimate(
            flops=flops, bytes_accessed=14 * 2**20, transcendentals=PER * rows * seq
        ),
        compiler_params=pltpu.CompilerParams(
            dimension_semantics=("arbitrary",), vmem_limit_bytes=56 * 2**20
        ),
    )(queries, *pieces, weight)


def gate_kernel(heads_ref, gate_ref, gain_ref, out_ref, gated):
    total = jnp.zeros((OWN, 1), F32)
    width = PER * VDIM
    for group in range(GROUPS):
        columns = slice(group * width, (group + 1) * width)
        v = gate_ref[:, columns].astype(F32)
        part = heads_ref[group].astype(F32) * (v * jax.nn.sigmoid(v))
        gated[:, columns] = part
        total += jnp.sum(part * part, axis=-1, keepdims=True)
    scale = lax.rsqrt(total / (HEADS * VDIM) + EPS)
    for group in range(GROUPS):
        columns = slice(group * width, (group + 1) * width)
        out_ref[:, columns] = (gated[:, columns] * scale * gain_ref[:, columns]).astype(BF16)


def gate_and_norm(heads, gate, gain):
    return pl.pallas_call(
        gate_kernel,
        out_shape=jax.ShapeDtypeStruct((OWN, HEADS * VDIM), BF16),
        scratch_shapes=[pltpu.VMEM((OWN, HEADS * VDIM), F32)],
        cost_estimate=pl.CostEstimate(flops=10**7, bytes_accessed=3 * 2**20, transcendentals=0),
    )(heads, gate, gain)


def shifted(value, axis, by):
    length = lax.axis_size(axis)
    return lax.ppermute(value, axis, [(i, (i + by) % length) for i in range(length)])


def ring(value, axis):
    length = lax.axis_size(axis)
    ahead, behind, blocks = value, value, [value]
    for _ in range(length // 2 - 1):
        ahead, behind = shifted(ahead, axis, 1), shifted(behind, axis, -1)
        blocks += [ahead, behind]
    half = value.shape[0] // 2
    return blocks + [shifted(ahead[:half], axis, 1), shifted(behind[half:], axis, -1)]


def along(move, mesh_shape):
    zh_n, zl_n, y_n, x_n, core_n = mesh_shape
    pairs = []
    for zh in range(zh_n):
        for zl in range(zl_n):
            for y in range(y_n):
                group = zl * y_n + y
                column = ((zh * zl_n + zl) * y_n + y) * x_n * core_n
                for source, target in move(group // core_n, group % core_n, x_n):
                    pairs.append((column + source, column + target))
    return pairs


def shard_of_group(weight, mesh_shape):
    def one_way(by):
        return along(lambda x, c, n: [(x * 2 + c, (x + by) % n * 2 + c)], mesh_shape)

    def far(by):
        return along(
            lambda x, c, n: [((x + by) % n * 2 + c, (x + 2) % n * 2 + c)], mesh_shape
        )

    swap = along(lambda x, c, n: [(i * 2 + c, i * 2 + 1 - c) for i in range(n)], mesh_shape)
    group = lax.axis_index("zl") * lax.axis_size("y") + lax.axis_index("y")
    mine = lax.axis_index(DP) == group
    half = weight.shape[0] // 2
    right = lax.ppermute(weight, EVERY, one_way(1))
    left = lax.ppermute(weight, EVERY, one_way(-1))
    opposite = jnp.concatenate(
        [
            lax.ppermute(right[:half], EVERY, far(1)),
            lax.ppermute(left[half:], EVERY, far(-1)),
        ]
    )
    held = jnp.where(mine, weight, right + left + opposite)
    other = lax.ppermute(held, EVERY, swap)
    return jnp.where(lax.axis_index("core") == group % 2, held, other)


def per_device(mesh_shape, queries, latent, rope_key, latent_gain, kv_weight, gate, out_gain):
    block = lax.axis_index(("zh", "zl", "y"))
    position = block * OWN + jnp.arange(OWN, dtype=jnp.int32)
    half = ROPE // 2
    inverse = THETA ** (-jnp.arange(half, dtype=F32) / half)
    angles = position.astype(F32)[:, None] * inverse[None, :]
    cosine, sine = jnp.cos(angles), jnp.sin(angles)
    cosine = jnp.concatenate([cosine] * 4, axis=1)
    sine = jnp.concatenate([-sine, sine] * 2, axis=1)

    weight = shard_of_group(kv_weight, mesh_shape)
    sent = small_call(latent_kernel, (OWN, WIDE), 10**6, 2**20)(
        latent, rope_key, latent_gain[None, :], cosine, sine
    )
    head_queries = small_call(query_kernel, (GROUPS, OWN, QCOLS), 10**7, 3 * 2**20)(
        queries, cosine, sine
    )
    head_queries = lax.all_to_all(head_queries, ("zl", "y"), 0, 0, tiled=True)

    along_z = jnp.concatenate(ring(sent[: OWN // 2], Z))
    along_y = jnp.concatenate(ring(sent[OWN // 2 :], "y"))
    pieces = ring(along_z, "y") + ring(along_y, Z)

    heads_out = attention(head_queries, pieces, weight)
    heads_out = lax.all_to_all(heads_out, ("zl", "y"), 0, 0, tiled=True)
    return gate_and_norm(heads_out, gate, out_gain[None, :])


def solution(mesh):
    x_n, z_n, y_n = mesh.shape["dp"] // 2, 8, mesh.shape["sp"] // 8
    mesh_shape = (z_n // 2, 2, y_n, x_n, 2)
    named = Mesh(mesh.devices.reshape(mesh_shape), EVERY)
    tokens = P(("x", "core", "zh", "zl", "y"), None)
    return jax.shard_map(
        functools.partial(per_device, mesh_shape),
        mesh=named,
        in_specs=(tokens, tokens, tokens, P(), P(None, DP), tokens, P()),
        out_specs=tokens,
        check_vma=False,
    )
```

```python
import functools
import math

import jax
import jax.numpy as jnp
from jax import lax
from jax.experimental import pallas as pl
from jax.experimental.pallas import tpu as pltpu
from jax.sharding import Mesh
from jax.sharding import PartitionSpec as P


HEADS = 32
NOPE = 128
ROPE = 64
VDIM = 128
QK = NOPE + ROPE
RANK = 1024
GROUPS = 8
PER = HEADS // GROUPS
OWN = 128
ROWS = GROUPS * OWN
WIDE = RANK + 2 * ROPE

EPS = 1e-06
THETA = 10000.0
SCALE2 = math.log2(math.e) / math.sqrt(QK)
F32 = jnp.float32
BF16 = jnp.bfloat16

Z = ("zh", "zl")
SP = ("zh", "zl", "y")
DP = ("x", "core")
EVERY = ("zh", "zl", "y", "x", "core")


def call(kernel, shape, flops, moved, transcendentals=0, limit=None, **rest):
    return pl.pallas_call(
        kernel,
        out_shape=jax.ShapeDtypeStruct(shape, BF16),
        cost_estimate=pl.CostEstimate(
            flops=flops, bytes_accessed=moved, transcendentals=transcendentals
        ),
        compiler_params=pltpu.CompilerParams(vmem_limit_bytes=limit),
        **rest,
    )


def latent_kernel(latent_ref, key_ref, gain_ref, cos_ref, sin_ref, sent_ref):
    wide = latent_ref[...].astype(F32)
    mean = jnp.mean(wide * wide, axis=-1, keepdims=True)
    sent_ref[:, :RANK] = (wide * lax.rsqrt(mean + EPS) * gain_ref[...]).astype(BF16)
    u1, u2 = key_ref[:, : ROPE // 2].astype(F32), key_ref[:, ROPE // 2 :].astype(F32)
    cosine, sine = cos_ref[...], sin_ref[...]
    turned = [u1 * cosine - u2 * sine, u2 * cosine + u1 * sine]
    turned.append(jnp.zeros((OWN, ROPE), F32))
    sent_ref[:, RANK:] = jnp.concatenate(turned, axis=1).astype(BF16)


def query_kernel(q_ref, cos_ref, sin_ref, sent_ref):
    cosine, sine = cos_ref[...].T, sin_ref[...].T
    for pair in range(HEADS // 2):
        both = jnp.concatenate(
            [q_ref[:, 384 * pair + 128 * i : 384 * pair + 128 * (i + 1)].T for i in range(3)], axis=0
        )
        for side in range(2):
            head = both[QK * side : QK * (side + 1)]
            group, local = divmod(2 * pair + side, PER)
            to = group % (GROUPS // 2), group // (GROUPS // 2), local
            sent_ref[*to, :NOPE] = head[:NOPE]
            u1 = head[NOPE : NOPE + ROPE // 2].astype(F32)
            u2 = head[NOPE + ROPE // 2 :].astype(F32)
            turned = jnp.concatenate([u1 * cosine - u2 * sine, u2 * cosine + u1 * sine], axis=0)
            sent_ref[*to, NOPE:] = turned.astype(BF16)


def attention_kernel(sizes, bq, bk, begins, ends, q_ref, *refs):
    pieces, refs = refs[: len(sizes)], refs[len(sizes) :]
    w_ref, refs = refs[0], refs[1:]
    if not begins:
        acc_in, m_in, refs = refs[0], refs[1], refs[2:]
    (out_ref, refs) = (refs[0], refs[1:]) if ends else (None, refs)
    acc, m_ref, kext, vt, s_ref, q = refs
    keys = kext.shape[0]

    row = lax.broadcasted_iota(jnp.int32, (16, keys), 0)
    vt[VDIM:, :] = jnp.where(row == 0, 1.0, 0.0).astype(BF16)
    start = 0
    for size, piece in zip(sizes, pieces):
        step = min(size, 512)
        for at in range(0, size, step):
            kv = jnp.dot(piece[at : at + step, :RANK], w_ref[...], preferred_element_type=F32)
            rows = slice(start, start + step)
            kext[rows, :NOPE] = kv[:, :NOPE].astype(BF16)
            kext[rows, NOPE:] = piece[at : at + step, RANK:]
            vt[:VDIM, rows] = kv[:, NOPE:].T.astype(BF16)
            start += step
    for source in range(GROUPS):
        q[:QK, source * OWN : (source + 1) * OWN] = q_ref[source, 0]
    q[QK:, :] = jnp.zeros((256 - QK, ROWS), BF16)
    if begins:
        m_ref[...] = jnp.full(m_ref.shape, -jnp.inf, F32)
        acc[...] = jnp.zeros(acc.shape, F32)
    else:
        m_ref[...] = m_in[...]
        acc[...] = acc_in[...]

    blocks = keys // bk
    steps = blocks * (ROWS // bq)

    def score(t):
        rows = pl.ds(pl.multiple_of(lax.rem(t, blocks) * bk, bk), bk)
        columns = pl.ds(pl.multiple_of(lax.div(t, blocks) * bq, bq), bq)
        return jnp.dot(kext[rows, :], q[:, columns], preferred_element_type=F32)

    s_ref[0] = score(0)

    def step(t, slot):
        s_ref[1 - slot] = score(jnp.minimum(t + 1, steps - 1))
        s = s_ref[slot]
        rows = pl.ds(pl.multiple_of(lax.rem(t, blocks) * bk, bk), bk)
        columns = pl.ds(pl.multiple_of(lax.div(t, blocks) * bq, bq), bq)
        m_old = m_ref[0, 0:1, columns]
        m_new = jnp.maximum(m_old, jnp.max(s, axis=0, keepdims=True))
        p = jnp.exp2((s - m_new) * SCALE2).astype(BF16)
        shrink = jnp.exp2((m_old - m_new) * SCALE2)
        acc[0, :, columns] = acc[0, :, columns] * shrink + jnp.dot(
            vt[:, rows], p, preferred_element_type=F32
        )
        m_ref[0, 0:1, columns] = m_new

    def two(i, carry):
        step(2 * i, 0)
        step(2 * i + 1, 1)
        return carry

    lax.fori_loop(0, steps // 2, two, 0)
    if ends:
        for source in range(GROUPS):
            part = acc[0, :, source * OWN : (source + 1) * OWN]
            out_ref[source] = (part[:VDIM] / part[VDIM : VDIM + 1]).T.astype(BF16)


def attention(queries, pieces, weight, state=(), ends=False, bq=512, bk=512):
    sizes = tuple(p.shape[0] for p in pieces)
    keys = sum(sizes)
    state_shapes = (PER, VDIM + 16, ROWS), (PER, 8, ROWS)
    state_specs = [pl.BlockSpec((1, *shape[1:]), lambda h: (h, 0, 0)) for shape in state_shapes]
    if ends:
        out_specs = pl.BlockSpec((GROUPS, OWN, VDIM), lambda h: (0, 0, h))
        out_shape = jax.ShapeDtypeStruct((GROUPS, OWN, PER * VDIM), BF16)
        kept = [pltpu.VMEM((1, *shape[1:]), F32) for shape in state_shapes]
    else:
        out_specs = state_specs
        out_shape = [jax.ShapeDtypeStruct(shape, F32) for shape in state_shapes]
        kept = []
    return pl.pallas_call(
        functools.partial(attention_kernel, sizes, bq, bk, not state, ends),
        grid=(PER,),
        in_specs=[pl.BlockSpec((GROUPS, 1, QK, OWN), lambda h: (0, h, 0, 0))]
        + [pl.BlockSpec((size, WIDE), lambda h: (0, 0)) for size in sizes]
        + [pl.BlockSpec((RANK, NOPE + VDIM), lambda h: (0, h))]
        + (state_specs if state else []),
        out_specs=out_specs,
        out_shape=out_shape,
        scratch_shapes=kept
        + [
            pltpu.VMEM((keys, 256), BF16),
            pltpu.VMEM((VDIM + 16, keys), BF16),
            pltpu.VMEM((2, bk, bq), F32),
            pltpu.VMEM((256, ROWS), BF16),
        ],
        cost_estimate=pl.CostEstimate(
            flops=2 * PER * keys * (RANK * 256 + ROWS * 768),
            bytes_accessed=keys * WIDE * 2 + 6 * 2**20,
            transcendentals=PER * ROWS * keys,
        ),
        compiler_params=pltpu.CompilerParams(
            dimension_semantics=("arbitrary",), vmem_limit_bytes=40 * 2**20
        ),
    )(queries, *pieces, weight, *state)


def gate_kernel(heads_ref, gate_ref, gain_ref, out_ref, gated):
    total = jnp.zeros((OWN, 1), F32)
    for group in range(GROUPS):
        columns = slice(group * PER * VDIM, (group + 1) * PER * VDIM)
        v = gate_ref[:, columns].astype(F32)
        part = heads_ref[group].astype(F32) * (v * jax.nn.sigmoid(v))
        gated[:, columns] = part
        total += jnp.sum(part * part, axis=-1, keepdims=True)
    scale = lax.rsqrt(total / (HEADS * VDIM) + EPS)
    for group in range(GROUPS):
        columns = slice(group * PER * VDIM, (group + 1) * PER * VDIM)
        out_ref[:, columns] = (gated[:, columns] * scale * gain_ref[:, columns]).astype(BF16)


def shifted(value, axis, by):
    length = lax.axis_size(axis)
    return lax.ppermute(value, axis, [(i, (i + by) % length) for i in range(length)])


def along(move, mesh_shape):
    zh_n, zl_n, y_n, x_n, core_n = mesh_shape
    pairs = []
    for column in range(zh_n * zl_n * y_n):
        group, first = column % (zl_n * y_n), column * x_n * core_n
        for source, target in move(group // core_n, group % core_n, x_n):
            pairs.append((first + source, first + target))
    return pairs


def shard_of_group(weight, mesh_shape):
    def one_way(by):
        return along(lambda x, c, n: [(x * 2 + c, (x + by) % n * 2 + c)], mesh_shape)

    def far(by):
        return along(lambda x, c, n: [((x + by) % n * 2 + c, (x + 2) % n * 2 + c)], mesh_shape)

    swap = along(lambda x, c, n: [(i * 2 + c, i * 2 + 1 - c) for i in range(n)], mesh_shape)
    group = lax.axis_index(("zl", "y"))
    mine = lax.axis_index(DP) == group
    half = weight.shape[0] // 2
    right = lax.ppermute(weight, EVERY, one_way(1))
    left = lax.ppermute(weight, EVERY, one_way(-1))
    after = yield
    right, left, after = lax.optimization_barrier((right, left, after))
    top = lax.ppermute(right[:half], EVERY, far(1))
    bottom = lax.ppermute(left[half:], EVERY, far(-1))
    after = yield after
    top, bottom, after = lax.optimization_barrier((top, bottom, after))
    held = jnp.where(mine, weight, right + left + jnp.concatenate([top, bottom]))
    other = lax.ppermute(held, EVERY, swap)
    yield jnp.where(lax.axis_index("core") == group % 2, held, other)


def per_device(mesh_shape, queries, latent, rope_key, latent_gain, kv_weight, gate, out_gain):
    position = lax.axis_index(SP) * OWN + jnp.arange(OWN, dtype=jnp.int32)
    half = ROPE // 2
    inverse = THETA ** (-jnp.arange(half, dtype=F32) / half)
    angles = position.astype(F32)[:, None] * inverse[None, :]
    cosine, sine = jnp.cos(angles), jnp.sin(angles)

    sent = call(latent_kernel, (OWN, WIDE), 10**6, 2**20)(
        latent, rope_key, latent_gain[None, :], cosine, sine
    )
    queries, kv_weight, sent = lax.optimization_barrier((queries, kv_weight, sent))
    head_queries = call(query_kernel, (GROUPS // 2, 2, PER, QK, OWN), 10**7, 3 * 2**20)(
        queries, cosine, sine
    )
    weight_steps = shard_of_group(kv_weight, mesh_shape)
    next(weight_steps)
    blocks, (ahead, behind) = [sent], (sent, sent)
    for step in range(3):
        ahead, behind = shifted(ahead, Z, 1), shifted(behind, Z, -1)
        blocks += [ahead, behind]
        if step == 0:
            head_queries, ahead, behind = lax.optimization_barrier((head_queries, ahead, behind))
    ahead, behind = weight_steps.send((ahead, behind))
    half = OWN // 2
    blocks += [shifted(ahead[:half], Z, 1), shifted(behind[half:], Z, -1)]
    column = jnp.concatenate(blocks)

    head_queries = lax.all_to_all(head_queries, "y", 0, 0, tiled=True)
    zl = lax.axis_index("zl")
    mine = jnp.where(zl == 0, head_queries[:, 0], head_queries[:, 1])
    other = jnp.where(zl == 0, head_queries[:, 1], head_queries[:, 0])
    other = shifted(other, "zl", 1)
    pair = jnp.where(zl == 0, mine, other), jnp.where(zl == 0, other, mine)
    head_queries = jnp.concatenate(pair)

    weight = weight_steps.send(column)
    state = attention(head_queries, [column], weight)
    ahead, behind = shifted(column, "y", 1), shifted(column, "y", -1)
    ahead, behind, state = lax.optimization_barrier((ahead, behind, state))
    far = [shifted(ahead[: ROWS // 2], "y", 1), shifted(behind[ROWS // 2 :], "y", -1)]
    state = attention(head_queries, [ahead, behind], weight, state)
    heads_out = attention(head_queries, far, weight, state, ends=True)
    heads_out = lax.all_to_all(heads_out, ("zl", "y"), 0, 0, tiled=True)
    return call(
        gate_kernel,
        (OWN, HEADS * VDIM),
        10**7,
        3 * 2**20,
        scratch_shapes=[pltpu.VMEM((OWN, HEADS * VDIM), F32)],
    )(heads_out, gate, out_gain[None, :])


def solution(mesh):
    x_n, z_n, y_n = mesh.shape["dp"] // 2, 8, mesh.shape["sp"] // 8
    mesh_shape = (z_n // 2, 2, y_n, x_n, 2)
    named = Mesh(mesh.devices.reshape(mesh_shape), EVERY)
    tokens = P(("x", "core", "zh", "zl", "y"), None)

    def body(*operands):
        return per_device(mesh_shape, *operands)

    return jax.shard_map(
        body,
        mesh=named,
        in_specs=(tokens, tokens, tokens, P(), P(None, DP), tokens, P()),
        out_specs=tokens,
        check_vma=False,
    )
```

```python
import functools
import math

import jax
import jax.numpy as jnp
from jax import lax
from jax.experimental import pallas as pl
from jax.experimental.pallas import tpu as pltpu
from jax.sharding import Mesh
from jax.sharding import PartitionSpec as P


HEADS = 32
NOPE = 128
ROPE = 64
VDIM = 128
QK = NOPE + ROPE
RANK = 1024
GROUPS = 8
PER = HEADS // GROUPS
OWN = 128
ROWS = GROUPS * OWN
BLOCK = OWN + OWN * ROPE // RANK

EPS = 1e-06
THETA = 10000.0
SCALE2 = math.log2(math.e) / math.sqrt(QK)
F32 = jnp.float32
BF16 = jnp.bfloat16

Z = ("zh", "zl")
SP = ("zh", "zl", "y")
DP = ("x", "core")
EVERY = ("zh", "zl", "y", "x", "core")


def call(kernel, shape, flops, moved, transcendentals=0, limit=None, **rest):
    return pl.pallas_call(
        kernel,
        out_shape=jax.ShapeDtypeStruct(shape, BF16),
        cost_estimate=pl.CostEstimate(
            flops=flops, bytes_accessed=moved, transcendentals=transcendentals
        ),
        compiler_params=pltpu.CompilerParams(vmem_limit_bytes=limit),
        **rest,
    )


def latent_kernel(latent_ref, key_ref, gain_ref, cos_ref, sin_ref, sent_ref):
    wide = latent_ref[...].astype(F32)
    mean = jnp.mean(wide * wide, axis=-1, keepdims=True)
    sent_ref[:OWN, :] = (wide * lax.rsqrt(mean + EPS) * gain_ref[...]).astype(BF16)
    key = key_ref[...].astype(F32).T
    u1, u2 = key[:, : ROPE // 2], key[:, ROPE // 2 :]
    cosine, sine = cos_ref[...], sin_ref[...]
    turned = jnp.concatenate([u1 * cosine - u2 * sine, u2 * cosine + u1 * sine], axis=1)
    pairs = jnp.concatenate([turned[: OWN // 2], turned[OWN // 2 :]], axis=1)
    packed = jnp.concatenate([pairs[i : i + 8] for i in range(0, OWN // 2, 8)], axis=1)
    sent_ref[OWN:, :] = packed.astype(BF16)


def query_kernel(q_ref, cos_ref, sin_ref, sent_ref):
    cosine, sine = cos_ref[...].T, sin_ref[...].T
    for pair in range(HEADS // 2):
        both = jnp.concatenate(
            [q_ref[:, 384 * pair + 128 * i : 384 * pair + 128 * (i + 1)].T for i in range(3)], axis=0
        )
        for side in range(2):
            head = both[QK * side : QK * (side + 1)]
            group, local = divmod(2 * pair + side, PER)
            to = group % (GROUPS // 2), group // (GROUPS // 2), local
            sent_ref[*to, :NOPE] = head[:NOPE]
            u1 = head[NOPE : NOPE + ROPE // 2].astype(F32)
            u2 = head[NOPE + ROPE // 2 :].astype(F32)
            turned = jnp.concatenate([u1 * cosine - u2 * sine, u2 * cosine + u1 * sine], axis=0)
            sent_ref[*to, NOPE:] = turned.astype(BF16)


def joined_kernel(*refs):
    start = 0
    for ref in refs[:-1]:
        refs[-1][start : start + ref.shape[0], :] = ref[...]
        start += ref.shape[0]


def joined(pieces):
    rows = sum(p.shape[0] for p in pieces)
    return call(joined_kernel, (rows, RANK), 10**6, 4 * rows * RANK)(*pieces)


def attention_kernel(sizes, bq, bk, begins, ends, q_ref, *refs):
    pieces, refs = refs[: len(sizes)], refs[len(sizes) :]
    w_ref, refs = refs[0], refs[1:]
    if not begins:
        acc_in, m_in, refs = refs[0], refs[1], refs[2:]
    (out_ref, refs) = (refs[0], refs[1:]) if ends else (None, refs)
    acc, m_ref, kext, vt, s_ref, q = refs
    keys = kext.shape[0]

    row = lax.broadcasted_iota(jnp.int32, (16, keys), 0)
    vt[VDIM:, :] = jnp.where(row == 0, 1.0, 0.0).astype(BF16)
    lane = lax.broadcasted_iota(jnp.int32, (OWN, 128), 1)
    start = 0
    for size, piece in zip(sizes, pieces):
        for at in range(0, size, 4 * BLOCK):
            step = min(4 * BLOCK, size - at)
            kv = jnp.dot(piece[at : at + step, :], w_ref[...], preferred_element_type=F32)
            for block in range(0, step, BLOCK):
                rows = slice(start, start + OWN)
                kext[rows, :NOPE] = kv[block : block + OWN, :NOPE].astype(BF16)
                vt[:VDIM, rows] = kv[block : block + OWN, NOPE:].T.astype(BF16)
                packed = piece[at + block + OWN : at + block + BLOCK, :].astype(F32)
                pairs = jnp.concatenate(
                    [packed[:, i : i + 128] for i in range(0, RANK, 128)], axis=0
                )
                both = jnp.concatenate([pairs, pltpu.roll(pairs, ROPE, 1)], axis=0)
                kext[rows, NOPE:] = jnp.where(lane < ROPE, both, 0.0).astype(BF16)
                start += OWN
    for source in range(GROUPS):
        q[:QK, source * OWN : (source + 1) * OWN] = q_ref[source, 0]
    q[QK:, :] = jnp.zeros((256 - QK, ROWS), BF16)
    if begins:
        m_ref[...] = jnp.full(m_ref.shape, -jnp.inf, F32)
        acc[...] = jnp.zeros(acc.shape, F32)
    else:
        m_ref[...] = m_in[...]
        acc[...] = acc_in[...]

    blocks = keys // bk
    steps = blocks * (ROWS // bq)

    def score(t):
        rows = pl.ds(pl.multiple_of(lax.rem(t, blocks) * bk, bk), bk)
        columns = pl.ds(pl.multiple_of(lax.div(t, blocks) * bq, bq), bq)
        return jnp.dot(kext[rows, :], q[:, columns], preferred_element_type=F32)

    s_ref[0] = score(0)

    def step(t, slot):
        s_ref[1 - slot] = score(jnp.minimum(t + 1, steps - 1))
        s = s_ref[slot]
        rows = pl.ds(pl.multiple_of(lax.rem(t, blocks) * bk, bk), bk)
        columns = pl.ds(pl.multiple_of(lax.div(t, blocks) * bq, bq), bq)
        m_old = m_ref[0, 0:1, columns]
        m_new = jnp.maximum(m_old, jnp.max(s, axis=0, keepdims=True))
        p = jnp.exp2((s - m_new) * SCALE2).astype(BF16)
        shrink = jnp.exp2((m_old - m_new) * SCALE2)
        acc[0, :, columns] = acc[0, :, columns] * shrink + jnp.dot(
            vt[:, rows], p, preferred_element_type=F32
        )
        m_ref[0, 0:1, columns] = m_new

    def two(i, carry):
        step(2 * i, 0)
        step(2 * i + 1, 1)
        return carry

    lax.fori_loop(0, steps // 2, two, 0)
    if ends:
        for source in range(GROUPS):
            part = acc[0, :, source * OWN : (source + 1) * OWN]
            out_ref[source] = (part[:VDIM] / part[VDIM : VDIM + 1]).T.astype(BF16)


def attention(queries, pieces, weight, state=(), ends=False, bq=512, bk=1024):
    sizes = tuple(p.shape[0] for p in pieces)
    keys = sum(sizes) // BLOCK * OWN
    state_shapes = (PER, VDIM + 16, ROWS), (PER, 8, ROWS)
    state_specs = [pl.BlockSpec((1, *shape[1:]), lambda h: (h, 0, 0)) for shape in state_shapes]
    if ends:
        out_specs = pl.BlockSpec((GROUPS, OWN, VDIM), lambda h: (0, 0, h))
        out_shape = jax.ShapeDtypeStruct((GROUPS, OWN, PER * VDIM), BF16)
        kept = [pltpu.VMEM((1, *shape[1:]), F32) for shape in state_shapes]
    else:
        out_specs = state_specs
        out_shape = [jax.ShapeDtypeStruct(shape, F32) for shape in state_shapes]
        kept = []
    return pl.pallas_call(
        functools.partial(attention_kernel, sizes, bq, bk, not state, ends),
        grid=(PER,),
        in_specs=[pl.BlockSpec((GROUPS, 1, QK, OWN), lambda h: (0, h, 0, 0))]
        + [pl.BlockSpec((size, RANK), lambda h: (0, 0)) for size in sizes]
        + [pl.BlockSpec((RANK, NOPE + VDIM), lambda h: (0, h))]
        + (state_specs if state else []),
        out_specs=out_specs,
        out_shape=out_shape,
        scratch_shapes=kept
        + [
            pltpu.VMEM((keys, 256), BF16),
            pltpu.VMEM((VDIM + 16, keys), BF16),
            pltpu.VMEM((2, bk, bq), F32),
            pltpu.VMEM((256, ROWS), BF16),
        ],
        cost_estimate=pl.CostEstimate(
            flops=2 * PER * keys * (RANK * 256 + ROWS * 768),
            bytes_accessed=sum(sizes) * RANK * 2 + 6 * 2**20,
            transcendentals=PER * ROWS * keys,
        ),
        compiler_params=pltpu.CompilerParams(
            dimension_semantics=("arbitrary",), vmem_limit_bytes=40 * 2**20
        ),
    )(queries, *pieces, weight, *state)


def gate_kernel(heads_ref, gate_ref, gain_ref, out_ref, gated):
    total = jnp.zeros((OWN, 1), F32)
    for group in range(GROUPS):
        columns = slice(group * PER * VDIM, (group + 1) * PER * VDIM)
        v = gate_ref[:, columns].astype(F32)
        part = heads_ref[group].astype(F32) * (v * jax.nn.sigmoid(v))
        gated[:, columns] = part
        total += jnp.sum(part * part, axis=-1, keepdims=True)
    scale = lax.rsqrt(total / (HEADS * VDIM) + EPS)
    for group in range(GROUPS):
        columns = slice(group * PER * VDIM, (group + 1) * PER * VDIM)
        out_ref[:, columns] = (gated[:, columns] * scale * gain_ref[:, columns]).astype(BF16)


def shifted(value, axis, by):
    length = lax.axis_size(axis)
    return lax.ppermute(value, axis, [(i, (i + by) % length) for i in range(length)])


def along(move, mesh_shape):
    zh_n, zl_n, y_n, x_n, core_n = mesh_shape
    pairs = []
    for column in range(zh_n * zl_n * y_n):
        group, first = column % (zl_n * y_n), column * x_n * core_n
        for source, target in move(group // core_n, group % core_n, x_n):
            pairs.append((first + source, first + target))
    return pairs


def pick_kernel(role_ref, own, right, left, top, bottom, out_ref, sem):
    half = out_ref.shape[0] // 2
    for role, source in ((0, own), (1, right), (3, left)):

        @pl.when(role_ref[0] == role)
        def _(source=source):
            copy = pltpu.make_async_copy(source, out_ref, sem.at[0])
            copy.start()
            copy.wait()

    @pl.when(role_ref[0] == 2)
    def _():
        first = pltpu.make_async_copy(top, out_ref.at[:half], sem.at[0])
        second = pltpu.make_async_copy(bottom, out_ref.at[half:], sem.at[1])
        first.start()
        second.start()
        first.wait()
        second.wait()


def picked(role, *sources):
    return call(
        pick_kernel,
        sources[0].shape,
        10**6,
        2 * sources[0].size,
        in_specs=[pl.BlockSpec(memory_space=pltpu.SMEM)]
        + [pl.BlockSpec(memory_space=pl.ANY)] * len(sources),
        out_specs=pl.BlockSpec(memory_space=pltpu.VMEM),
        scratch_shapes=[pltpu.SemaphoreType.DMA((2,))],
    )(role[None], *sources)


def shard_of_group(weight, mesh_shape):
    def one_way(by):
        return along(lambda x, c, n: [(x * 2 + c, (x + by) % n * 2 + c)], mesh_shape)

    def far(by):
        return along(lambda x, c, n: [((x + by) % n * 2 + c, (x + 2) % n * 2 + c)], mesh_shape)

    swap = along(lambda x, c, n: [(i * 2 + c, i * 2 + 1 - c) for i in range(n)], mesh_shape)
    group = lax.axis_index(("zl", "y"))
    half = weight.shape[0] // 2
    right = lax.ppermute(weight, EVERY, one_way(1))
    left = lax.ppermute(weight, EVERY, one_way(-1))
    right, left = lax.optimization_barrier((right, left))
    top = lax.ppermute(right[:half], EVERY, far(1))
    bottom = lax.ppermute(left[half:], EVERY, far(-1))
    after = yield
    top, bottom, after = lax.optimization_barrier((top, bottom, after))
    step_from = jnp.where(lax.axis_index("core") == group % 2, lax.axis_index("x") - group // 2, 0)
    role = lax.rem(step_from + mesh_shape[3], mesh_shape[3])
    held = picked(role, weight, right, left, top, bottom)
    other = lax.ppermute(held, EVERY, swap)
    yield jnp.where(lax.axis_index("core") == group % 2, held, other)


def per_device(mesh_shape, queries, latent, rope_key, latent_gain, kv_weight, gate, out_gain):
    position = lax.axis_index(SP) * OWN + jnp.arange(OWN, dtype=jnp.int32)
    half = ROPE // 2
    inverse = THETA ** (-jnp.arange(half, dtype=F32) / half)
    angles = position.astype(F32)[:, None] * inverse[None, :]
    cosine, sine = jnp.cos(angles), jnp.sin(angles)

    sent = call(latent_kernel, (BLOCK, RANK), 10**6, 2**20)(
        latent, rope_key.T, latent_gain[None, :], cosine, sine
    )
    queries, kv_weight, sent = lax.optimization_barrier((queries, kv_weight, sent))
    head_queries = call(query_kernel, (GROUPS // 2, 2, PER, QK, OWN), 10**7, 3 * 2**20)(
        queries, cosine, sine
    )
    weight_steps = shard_of_group(kv_weight, mesh_shape)
    next(weight_steps)
    head_queries = lax.all_to_all(head_queries, "y", 0, 0, tiled=True)
    blocks, (ahead, behind) = [sent], (sent, sent)
    for _ in range(3):
        ahead, behind = shifted(ahead, Z, 1), shifted(behind, Z, -1)
        blocks += [ahead, behind]
    half = BLOCK // 2 + 4
    blocks += [shifted(ahead[:half], Z, 1), shifted(behind[half:], Z, -1)]
    first, second = joined(blocks[:4]), joined(blocks[4:])

    zl = lax.axis_index("zl")
    mine = jnp.where(zl == 0, head_queries[:, 0], head_queries[:, 1])
    other = jnp.where(zl == 0, head_queries[:, 1], head_queries[:, 0])
    other = shifted(other, "zl", 1)
    pair = jnp.where(zl == 0, mine, other), jnp.where(zl == 0, other, mine)
    head_queries = jnp.concatenate(pair)

    weight = weight_steps.send(second)
    beside0 = [shifted(first, "y", 1), shifted(first, "y", -1)]
    beside1 = [shifted(second, "y", 1), shifted(second, "y", -1)]
    opposite = [shifted(beside0[0], "y", 1), shifted(beside1[1], "y", -1)]
    state = attention(head_queries, [first, second], weight)
    state = attention(head_queries, beside0 + beside1, weight, state)
    heads_out = attention(head_queries, opposite, weight, state, ends=True)
    heads_out = lax.all_to_all(heads_out, ("zl", "y"), 0, 0, tiled=True)
    return call(
        gate_kernel,
        (OWN, HEADS * VDIM),
        10**7,
        3 * 2**20,
        scratch_shapes=[pltpu.VMEM((OWN, HEADS * VDIM), F32)],
    )(heads_out, gate, out_gain[None, :])


def solution(mesh):
    x_n, z_n, y_n = mesh.shape["dp"] // 2, 8, mesh.shape["sp"] // 8
    mesh_shape = (z_n // 2, 2, y_n, x_n, 2)
    named = Mesh(mesh.devices.reshape(mesh_shape), EVERY)
    tokens = P(("x", "core", "zh", "zl", "y"), None)

    def body(*operands):
        return per_device(mesh_shape, *operands)

    return jax.shard_map(
        body,
        mesh=named,
        in_specs=(tokens, tokens, tokens, P(), P(None, DP), tokens, P()),
        out_specs=tokens,
        check_vma=False,
    )
```

```python
import functools
import math

import jax
import jax.numpy as jnp
from jax import lax
from jax.experimental import pallas as pl
from jax.experimental.pallas import tpu as pltpu
from jax.sharding import Mesh
from jax.sharding import PartitionSpec as P


HEADS = 32
NOPE = 128
ROPE = 64
VDIM = 128
QK = NOPE + ROPE
RANK = 1024
GROUPS = 8
PER = HEADS // GROUPS
OWN = 128
ROWS = GROUPS * OWN
BLOCK = OWN + OWN * ROPE // RANK

EPS = 1e-06
THETA = 10000.0
SCALE2 = math.log2(math.e) / math.sqrt(QK)
F32 = jnp.float32
BF16 = jnp.bfloat16

Z = ("zh", "zl")
SP = ("zh", "zl", "y")
DP = ("x", "core")
EVERY = ("zh", "zl", "y", "x", "core")


def call(kernel, shape, flops, moved, transcendentals=0, limit=None, **rest):
    return pl.pallas_call(
        kernel,
        out_shape=jax.ShapeDtypeStruct(shape, BF16),
        cost_estimate=pl.CostEstimate(
            flops=flops, bytes_accessed=moved, transcendentals=transcendentals
        ),
        compiler_params=pltpu.CompilerParams(vmem_limit_bytes=limit),
        **rest,
    )


def latent_kernel(latent_ref, key_ref, gain_ref, cos_ref, sin_ref, sent_ref):
    wide = latent_ref[...].astype(F32)
    mean = jnp.mean(wide * wide, axis=-1, keepdims=True)
    sent_ref[:OWN, :] = (wide * lax.rsqrt(mean + EPS) * gain_ref[...]).astype(BF16)
    key = key_ref[...].astype(F32).T
    u1, u2 = key[:, : ROPE // 2], key[:, ROPE // 2 :]
    cosine, sine = cos_ref[...], sin_ref[...]
    turned = jnp.concatenate([u1 * cosine - u2 * sine, u2 * cosine + u1 * sine], axis=1)
    pairs = jnp.concatenate([turned[: OWN // 2], turned[OWN // 2 :]], axis=1)
    packed = jnp.concatenate([pairs[i : i + 8] for i in range(0, OWN // 2, 8)], axis=1)
    sent_ref[OWN:, :] = packed.astype(BF16)


def query_kernel(q_ref, cos_ref, sin_ref, sent_ref):
    cosine, sine = cos_ref[...].T, sin_ref[...].T
    for pair in range(HEADS // 2):
        both = jnp.concatenate(
            [q_ref[:, 384 * pair + 128 * i : 384 * pair + 128 * (i + 1)].T for i in range(3)], axis=0
        )
        for side in range(2):
            head = both[QK * side : QK * (side + 1)]
            group, local = divmod(2 * pair + side, PER)
            to = group % (GROUPS // 2), group // (GROUPS // 2), local
            sent_ref[*to, :NOPE] = head[:NOPE]
            u1 = head[NOPE : NOPE + ROPE // 2].astype(F32)
            u2 = head[NOPE + ROPE // 2 :].astype(F32)
            turned = jnp.concatenate([u1 * cosine - u2 * sine, u2 * cosine + u1 * sine], axis=0)
            sent_ref[*to, NOPE:] = turned.astype(BF16)


def joined_kernel(*refs):
    start = 0
    for ref in refs[:-1]:
        refs[-1][start : start + ref.shape[0], :] = ref[...]
        start += ref.shape[0]


def joined(pieces):
    rows = sum(p.shape[0] for p in pieces)
    return call(joined_kernel, (rows, RANK), 10**6, 4 * rows * RANK)(*pieces)


def attention_kernel(sizes, bq, bk, begins, ends, q_ref, *refs):
    pieces, refs = refs[: len(sizes)], refs[len(sizes) :]
    w_ref, refs = refs[0], refs[1:]
    if not begins:
        acc_in, m_in, refs = refs[0], refs[1], refs[2:]
    (out_ref, refs) = (refs[0], refs[1:]) if ends else (None, refs)
    acc, m_ref, kext, vt, s_ref, q = refs
    keys = kext.shape[0]

    row = lax.broadcasted_iota(jnp.int32, (16, keys), 0)
    vt[VDIM:, :] = jnp.where(row == 0, 1.0, 0.0).astype(BF16)
    lane = lax.broadcasted_iota(jnp.int32, (OWN, 128), 1)
    start = 0
    for size, piece in zip(sizes, pieces):
        for at in range(0, size, 4 * BLOCK):
            step = min(4 * BLOCK, size - at)
            kv = jnp.dot(piece[at : at + step, :], w_ref[...], preferred_element_type=F32)
            for block in range(0, step, BLOCK):
                rows = slice(start, start + OWN)
                kext[rows, :NOPE] = kv[block : block + OWN, :NOPE].astype(BF16)
                vt[:VDIM, rows] = kv[block : block + OWN, NOPE:].T.astype(BF16)
                packed = piece[at + block + OWN : at + block + BLOCK, :].astype(F32)
                pairs = jnp.concatenate(
                    [packed[:, i : i + 128] for i in range(0, RANK, 128)], axis=0
                )
                both = jnp.concatenate([pairs, pltpu.roll(pairs, ROPE, 1)], axis=0)
                kext[rows, NOPE:] = jnp.where(lane < ROPE, both, 0.0).astype(BF16)
                start += OWN
    for source in range(GROUPS):
        q[:QK, source * OWN : (source + 1) * OWN] = q_ref[source, 0]
    q[QK:, :] = jnp.zeros((256 - QK, ROWS), BF16)
    if begins:
        m_ref[...] = jnp.full(m_ref.shape, -jnp.inf, F32)
        acc[...] = jnp.zeros(acc.shape, F32)
    else:
        m_ref[...] = m_in[...]
        acc[...] = acc_in[...]

    blocks = keys // bk
    steps = blocks * (ROWS // bq)

    def score(t):
        rows = pl.ds(pl.multiple_of(lax.rem(t, blocks) * bk, bk), bk)
        columns = pl.ds(pl.multiple_of(lax.div(t, blocks) * bq, bq), bq)
        return jnp.dot(kext[rows, :], q[:, columns], preferred_element_type=F32)

    s_ref[0] = score(0)

    def step(t, slot):
        s_ref[1 - slot] = score(jnp.minimum(t + 1, steps - 1))
        s = s_ref[slot]
        rows = pl.ds(pl.multiple_of(lax.rem(t, blocks) * bk, bk), bk)
        columns = pl.ds(pl.multiple_of(lax.div(t, blocks) * bq, bq), bq)
        m_old = m_ref[0, 0:1, columns]
        m_new = jnp.maximum(m_old, jnp.max(s, axis=0, keepdims=True))
        p = jnp.exp2((s - m_new) * SCALE2).astype(BF16)
        shrink = jnp.exp2((m_old - m_new) * SCALE2)
        acc[0, :, columns] = acc[0, :, columns] * shrink + jnp.dot(
            vt[:, rows], p, preferred_element_type=F32
        )
        m_ref[0, 0:1, columns] = m_new

    def two(i, carry):
        step(2 * i, 0)
        step(2 * i + 1, 1)
        return carry

    lax.fori_loop(0, steps // 2, two, 0)
    if ends:
        for source in range(GROUPS):
            part = acc[0, :, source * OWN : (source + 1) * OWN]
            out_ref[source] = (part[:VDIM] / part[VDIM : VDIM + 1]).T.astype(BF16)


def attention(queries, pieces, weight, state=(), ends=False, bq=512):
    sizes = tuple(p.shape[0] for p in pieces)
    keys = sum(sizes) // BLOCK * OWN
    bk = 1024 if keys % 1536 else 1536
    state_shapes = (PER, VDIM + 16, ROWS), (PER, 8, ROWS)
    state_specs = [pl.BlockSpec((1, *shape[1:]), lambda h: (h, 0, 0)) for shape in state_shapes]
    if ends:
        out_specs = pl.BlockSpec((GROUPS, OWN, VDIM), lambda h: (0, 0, h))
        out_shape = jax.ShapeDtypeStruct((GROUPS, OWN, PER * VDIM), BF16)
        kept = [pltpu.VMEM((1, *shape[1:]), F32) for shape in state_shapes]
    else:
        out_specs = state_specs
        out_shape = [jax.ShapeDtypeStruct(shape, F32) for shape in state_shapes]
        kept = []
    return pl.pallas_call(
        functools.partial(attention_kernel, sizes, bq, bk, not state, ends),
        grid=(PER,),
        in_specs=[pl.BlockSpec((GROUPS, 1, QK, OWN), lambda h: (0, h, 0, 0))]
        + [pl.BlockSpec((size, RANK), lambda h: (0, 0)) for size in sizes]
        + [pl.BlockSpec((RANK, NOPE + VDIM), lambda h: (0, h))]
        + (state_specs if state else []),
        out_specs=out_specs,
        out_shape=out_shape,
        scratch_shapes=kept
        + [
            pltpu.VMEM((keys, 256), BF16),
            pltpu.VMEM((VDIM + 16, keys), BF16),
            pltpu.VMEM((2, bk, bq), F32),
            pltpu.VMEM((256, ROWS), BF16),
        ],
        cost_estimate=pl.CostEstimate(
            flops=2 * PER * keys * (RANK * 256 + ROWS * 768),
            bytes_accessed=sum(sizes) * RANK * 2 + 6 * 2**20,
            transcendentals=PER * ROWS * keys,
        ),
        compiler_params=pltpu.CompilerParams(
            dimension_semantics=("arbitrary",), vmem_limit_bytes=40 * 2**20
        ),
    )(queries, *pieces, weight, *state)


def gate_kernel(heads_ref, gate_ref, gain_ref, out_ref, gated):
    total = jnp.zeros((OWN, 1), F32)
    for group in range(GROUPS):
        columns = slice(group * PER * VDIM, (group + 1) * PER * VDIM)
        v = gate_ref[:, columns].astype(F32)
        part = heads_ref[group].astype(F32) * (v * jax.nn.sigmoid(v))
        gated[:, columns] = part
        total += jnp.sum(part * part, axis=-1, keepdims=True)
    scale = lax.rsqrt(total / (HEADS * VDIM) + EPS)
    for group in range(GROUPS):
        columns = slice(group * PER * VDIM, (group + 1) * PER * VDIM)
        out_ref[:, columns] = (gated[:, columns] * scale * gain_ref[:, columns]).astype(BF16)


def shifted(value, axis, by):
    length = lax.axis_size(axis)
    return lax.ppermute(value, axis, [(i, (i + by) % length) for i in range(length)])


def along(move, mesh_shape):
    zh_n, zl_n, y_n, x_n, core_n = mesh_shape
    pairs = []
    for column in range(zh_n * zl_n * y_n):
        group, first = column % (zl_n * y_n), column * x_n * core_n
        for source, target in move(group // core_n, group % core_n, x_n):
            pairs.append((first + source, first + target))
    return pairs


def pick_kernel(role_ref, own, right, left, top, bottom, out_ref, sem):
    half = out_ref.shape[0] // 2
    for role, source in ((0, own), (1, right), (3, left)):

        @pl.when(role_ref[0] == role)
        def _(source=source):
            copy = pltpu.make_async_copy(source, out_ref, sem.at[0])
            copy.start()
            copy.wait()

    @pl.when(role_ref[0] == 2)
    def _():
        first = pltpu.make_async_copy(top, out_ref.at[:half], sem.at[0])
        second = pltpu.make_async_copy(bottom, out_ref.at[half:], sem.at[1])
        first.start()
        second.start()
        first.wait()
        second.wait()


def picked(role, *sources):
    return call(
        pick_kernel,
        sources[0].shape,
        10**6,
        2 * sources[0].size,
        in_specs=[pl.BlockSpec(memory_space=pltpu.SMEM)]
        + [pl.BlockSpec(memory_space=pl.ANY)] * len(sources),
        out_specs=pl.BlockSpec(memory_space=pltpu.VMEM),
        scratch_shapes=[pltpu.SemaphoreType.DMA((2,))],
    )(role[None], *sources)


def shard_of_group(weight, mesh_shape):
    def one_way(by):
        return along(lambda x, c, n: [(x * 2 + c, (x + by) % n * 2 + c)], mesh_shape)

    def far(by):
        return along(lambda x, c, n: [((x + by) % n * 2 + c, (x + 2) % n * 2 + c)], mesh_shape)

    swap = along(lambda x, c, n: [(i * 2 + c, i * 2 + 1 - c) for i in range(n)], mesh_shape)
    group = lax.axis_index(("zl", "y"))
    half = weight.shape[0] // 2
    right = lax.ppermute(weight, EVERY, one_way(1))
    left = lax.ppermute(weight, EVERY, one_way(-1))
    right, left = lax.optimization_barrier((right, left))
    top = lax.ppermute(right[:half], EVERY, far(1))
    bottom = lax.ppermute(left[half:], EVERY, far(-1))
    after = yield
    top, bottom, after = lax.optimization_barrier((top, bottom, after))
    step_from = jnp.where(lax.axis_index("core") == group % 2, lax.axis_index("x") - group // 2, 0)
    role = lax.rem(step_from + mesh_shape[3], mesh_shape[3])
    held = picked(role, weight, right, left, top, bottom)
    other = lax.ppermute(held, EVERY, swap)
    yield jnp.where(lax.axis_index("core") == group % 2, held, other)


def per_device(mesh_shape, queries, latent, rope_key, latent_gain, kv_weight, gate, out_gain):
    position = lax.axis_index(SP) * OWN + jnp.arange(OWN, dtype=jnp.int32)
    half = ROPE // 2
    inverse = THETA ** (-jnp.arange(half, dtype=F32) / half)
    angles = position.astype(F32)[:, None] * inverse[None, :]
    cosine, sine = jnp.cos(angles), jnp.sin(angles)

    sent = call(latent_kernel, (BLOCK, RANK), 10**6, 2**20)(
        latent, rope_key.T, latent_gain[None, :], cosine, sine
    )
    queries, kv_weight, sent = lax.optimization_barrier((queries, kv_weight, sent))
    head_queries = call(query_kernel, (GROUPS // 2, 2, PER, QK, OWN), 10**7, 3 * 2**20)(
        queries, cosine, sine
    )
    weight_steps = shard_of_group(kv_weight, mesh_shape)
    next(weight_steps)
    head_queries = lax.all_to_all(head_queries, "y", 0, 0, tiled=True)
    blocks, (ahead, behind) = [sent], (sent, sent)
    for _ in range(3):
        ahead, behind = shifted(ahead, Z, 1), shifted(behind, Z, -1)
        blocks += [ahead, behind]
    half = BLOCK // 2 + 4
    blocks += [shifted(ahead[:half], Z, 1), shifted(behind[half:], Z, -1)]
    first, second = joined(blocks[:4]), joined(blocks[4:])

    zl = lax.axis_index("zl")
    mine = jnp.where(zl == 0, head_queries[:, 0], head_queries[:, 1])
    other = jnp.where(zl == 0, head_queries[:, 1], head_queries[:, 0])
    other = shifted(other, "zl", 1)
    pair = jnp.where(zl == 0, mine, other), jnp.where(zl == 0, other, mine)
    head_queries = jnp.concatenate(pair)

    weight = weight_steps.send(second)
    beside0 = [shifted(first, "y", 1), shifted(first, "y", -1)]
    beside1 = [shifted(second, "y", 1), shifted(second, "y", -1)]
    opposite = [shifted(beside0[0], "y", 1), shifted(beside1[1], "y", -1)]
    state = attention(head_queries, [first, second, *beside0, *beside1], weight)
    heads_out = attention(head_queries, opposite, weight, state, ends=True)
    heads_out = lax.all_to_all(heads_out, ("zl", "y"), 0, 0, tiled=True)
    return call(
        gate_kernel,
        (OWN, HEADS * VDIM),
        10**7,
        3 * 2**20,
        scratch_shapes=[pltpu.VMEM((OWN, HEADS * VDIM), F32)],
    )(heads_out, gate, out_gain[None, :])


def solution(mesh):
    x_n, z_n, y_n = mesh.shape["dp"] // 2, 8, mesh.shape["sp"] // 8
    mesh_shape = (z_n // 2, 2, y_n, x_n, 2)
    named = Mesh(mesh.devices.reshape(mesh_shape), EVERY)
    tokens = P(("x", "core", "zh", "zl", "y"), None)

    def body(*operands):
        return per_device(mesh_shape, *operands)

    return jax.shard_map(
        body,
        mesh=named,
        in_specs=(tokens, tokens, tokens, P(), P(None, DP), tokens, P()),
        out_specs=tokens,
        check_vma=False,
    )
```
